32 devices in a mesh: sp: 4 (over z), fs: 4 (over y, x), tp: 2 (over core).
Axes of the slice: x: 2, y: 2, z: 4, core: 2. Of those that a mesh axis runs over, the one named last changes fastest.
Arguments:
- tokens: bfloat16 [16384, 2048], P(('fs', 'sp', 'tp')), parts along dimension 0, may hold values from -6 to 6
- norm_gain: float32 [2048], replicated, may hold values from 0.1 to 1.9
- w_pool: bfloat16 [2048, 1024], P(None, 'tp'), may hold values from -0.125 to 0.125
- w_query: bfloat16 [2048, 1024], P(None, 'tp'), may hold values from -0.125 to 0.125
- w_key: bfloat16 [2048, 1024], P(None, 'tp'), may hold values from -0.125 to 0.125
- w_value: bfloat16 [2048, 1024], P(None, 'tp'), may hold values from -0.125 to 0.125
- w_gate: bfloat16 [2048, 1024], P(None, 'tp'), may hold values from -0.125 to 0.125
- pool_mix: bfloat16 [4, 256, 256], P('tp'), may hold values from -0.375 to 0.375
- pool_bias: float32 [4, 256], P('tp'), may hold values from -3 to 3
- pool_gain: float32 [1024], P('tp'), may hold values from 0.1 to 1.9
- ret_gain: float32 [1024], P('tp'), may hold values from 0.1 to 1.9
- w_out_pool: bfloat16 [1024, 2048], P('tp'), may hold values from -0.125 to 0.125
- w_out_ret: bfloat16 [1024, 2048], P('tp'), may hold values from -0.125 to 0.125
Outputs:
- mixed: bfloat16 [16384, 2048], P(('fs', 'sp', 'tp')), parts along dimension 0
The draws below stay inside these ranges and needn't reach their ends.
There are 4 independent parts, one for each index of `fs`. The reference program is written for one: setup_inputs(seed, part) draws one part's arguments, and reference() takes and returns one part's arrays. A program takes and returns all parts, laid end to end along the dimension named above; an argument that names none is the same for every part. Nothing has to cross between parts.
All inputs are finite; a program needn't handle non-finite values.
Results may differ from the reference program's by a relative error of at most 0.012.
Values may be sent and summed in bfloat16 or wider, within the bound.
A program may use at most 128 MiB of HBM per device.

```python
import jax
import jax.numpy as jnp
from jax import lax

D = 2048
GROUP_DIM = 256
POOL_WIDTH = 1024
HEADS = 8
HEAD_DIM = 128
RET_WIDTH = 1024
BLOCK = 128
SEQ = 4096
N_TP = 2


def level_of(own_key, shape, cuts, smallest, high):
    factor_of, own = 1.0, jax.random.fold_in(own_key, 6)
    for dim, shards_of in cuts:
        steps = jnp.exp(jax.random.uniform(jax.random.fold_in(own, dim), (shards_of,), jnp.float32, smallest / len(cuts), high / len(cuts)))
        factor_of = factor_of * jnp.repeat(steps, shape[dim] // shards_of).reshape([-1 if axis == dim else 1 for axis in range(len(shape))])
    return factor_of


def noise(rng, extent, width, bound, cuts=(), kind=jnp.bfloat16):
    level = level_of(rng, extent, cuts, -0.22, 0.18) if cuts else 1.0
    entries = jax.random.normal(rng, extent, jnp.float32) * width * level
    return jnp.minimum(jnp.maximum(entries, -bound), bound).astype(kind)


def setup_inputs(seed: int = 0, part: int = 0) -> dict:
    splits = jax.random.split(jax.random.key(seed), 14)
    part_splits = jax.random.split(jax.random.fold_in(splits[13], part), 14)
    return {
        "tokens": noise(part_splits[0], (SEQ, D), 1.0, 6.0, ((0, 8),)),
        "norm_gain": jnp.clip(1.0 + 0.18 * jax.random.normal(splits[1], (D,), jnp.float32), 0.1, 1.9),
        "w_pool": noise(splits[2], (D, POOL_WIDTH), D ** -0.5, 0.125, ((1, 2),)),
        "w_query": noise(splits[3], (D, RET_WIDTH), D ** -0.5, 0.125, ((1, 2),)),
        "w_key": noise(splits[4], (D, RET_WIDTH), D ** -0.5, 0.125, ((1, 2),)),
        "w_value": noise(splits[5], (D, RET_WIDTH), D ** -0.5, 0.125, ((1, 2),)),
        "w_gate": noise(splits[6], (D, RET_WIDTH), D ** -0.5, 0.125, ((1, 2),)),
        "pool_mix": noise(splits[7], (4, GROUP_DIM, GROUP_DIM), GROUP_DIM ** -0.5, 0.375, ((0, 2),)),
        "pool_bias": noise(splits[8], (4, GROUP_DIM), 0.5, 3.0, ((0, 2),), jnp.float32),
        "pool_gain": jnp.clip(1.0 + 0.18 * jax.random.normal(splits[9], (POOL_WIDTH,), jnp.float32), 0.1, 1.9),
        "ret_gain": jnp.clip(1.0 + 0.18 * jax.random.normal(splits[10], (RET_WIDTH,), jnp.float32), 0.1, 1.9),
        "w_out_pool": noise(splits[11], (POOL_WIDTH, D), (POOL_WIDTH + RET_WIDTH) ** -0.5, 0.125, ((0, 2),)),
        "w_out_ret": noise(splits[12], (RET_WIDTH, D), (POOL_WIDTH + RET_WIDTH) ** -0.5, 0.125, ((0, 2),)),
    }


def rotary(values, positions):
    half = values.shape[-1] // 2
    inverse = 10000.0 ** (-jnp.arange(half, dtype=jnp.float32) / half)
    angles = positions[:, None] * inverse[None, :]
    cosine = jnp.cos(angles)[:, None, :]
    sine = jnp.sin(angles)[:, None, :]
    first = values[..., :half]
    second = values[..., half:]
    return jnp.concatenate([first * cosine - second * sine, second * cosine + first * sine], axis=-1)

def retain(query, key, value, log_decay):
    length = query.shape[0]
    blocks = length // BLOCK
    hp = lax.Precision.HIGHEST

    def split(values):
        return values.reshape(blocks, BLOCK, HEADS, HEAD_DIM).transpose(0, 2, 1, 3)
    steps = jnp.arange(BLOCK, dtype=jnp.float32)
    apart = steps[:, None] - steps[None, :]
    inner = jnp.where(apart[None] >= 0, jnp.exp(log_decay[:, None, None] * jnp.maximum(apart, 0.0)[None]), 0.0)
    query_decay = jnp.exp(log_decay[:, None] * (steps[None, :] + 1.0))
    key_decay = jnp.exp(log_decay[:, None] * (BLOCK - 1.0 - steps[None, :]))
    block_decay = jnp.exp(log_decay * BLOCK)

    def advance(state, pieces):
        qb, kb, vb = pieces
        scores = jnp.einsum('hid,hjd->hij', qb, kb, precision=hp) * inner
        out = jnp.einsum('hij,hje->hie', scores, vb, precision=hp)
        out = out + jnp.einsum('hid,hde->hie', qb, state, precision=hp) * query_decay[:, :, None]
        state = state * block_decay[:, None, None] + jnp.einsum('hjd,hje->hde', kb * key_decay[:, :, None], vb, precision=hp)
        return (state, out)
    start = jnp.zeros((HEADS, HEAD_DIM, HEAD_DIM), jnp.float32)
    state, outs = lax.scan(advance, start, (split(query), split(key), split(value)))
    return outs.transpose(0, 2, 1, 3).reshape(length, HEADS, HEAD_DIM)

def reference(tokens, norm_gain, w_pool, w_query, w_key, w_value, w_gate, pool_mix, pool_bias, pool_gain, ret_gain, w_out_pool, w_out_ret):
    xf = tokens.astype(jnp.float32)
    normed = (xf * lax.rsqrt(lax.optimization_barrier(jnp.mean(xf * xf, axis=-1, keepdims=True)) + 1e-06) * norm_gain).astype(jnp.bfloat16)
    pool_in = jnp.dot(normed, w_pool, preferred_element_type=jnp.float32).astype(jnp.bfloat16)
    query = jnp.dot(normed, w_query, preferred_element_type=jnp.float32).astype(jnp.bfloat16)
    key = jnp.dot(normed, w_key, preferred_element_type=jnp.float32).astype(jnp.bfloat16)
    value = jnp.dot(normed, w_value, preferred_element_type=jnp.float32).astype(jnp.bfloat16)
    gate = jnp.dot(normed, w_gate, preferred_element_type=jnp.float32).astype(jnp.bfloat16)
    positions = jnp.arange(SEQ, dtype=jnp.float32)
    groups = []
    for group in range(4):
        window = 2 ** (group + 1)
        block = pool_in[:, group * GROUP_DIM:(group + 1) * GROUP_DIM].astype(jnp.float32)
        running = jnp.cumsum(block, axis=0)
        padded = jnp.concatenate([jnp.zeros((window, GROUP_DIM), jnp.float32), running], axis=0)
        window_sum = padded[window:] - padded[:SEQ]
        count = jnp.minimum(positions + 1.0, float(window))[:, None]
        diff = (window_sum / count - block).astype(jnp.bfloat16)
        mixed_group = jnp.dot(diff, pool_mix[group], preferred_element_type=jnp.float32) + pool_bias[group][None, :]
        groups.append(mixed_group)
    pool_out = (jnp.concatenate(groups, axis=1) * pool_gain[None, :]).astype(jnp.bfloat16)
    head_ids = jnp.arange(HEADS, dtype=jnp.float32)
    log_decay = -2.0 ** (-5) * (SEQ / 16.0) ** (-2.0 * head_ids / (HEADS - 1))
    qf = rotary(query.astype(jnp.float32).reshape(SEQ, HEADS, HEAD_DIM), positions)
    kf = rotary(key.astype(jnp.float32).reshape(SEQ, HEADS, HEAD_DIM), positions) * HEAD_DIM ** (-0.5)
    vf = value.astype(jnp.float32).reshape(SEQ, HEADS, HEAD_DIM)
    raw = retain(qf, kf, vf, log_decay)
    mean = lax.optimization_barrier(jnp.mean(raw, axis=-1, keepdims=True))
    var = lax.optimization_barrier(jnp.mean(jnp.square(raw - mean), axis=-1, keepdims=True))
    normalized = ((raw - mean) * lax.rsqrt(var + 1e-06)).reshape(SEQ, RET_WIDTH) * ret_gain[None, :]
    ret_out = (jax.nn.silu(gate.astype(jnp.float32)) * normalized).astype(jnp.bfloat16)
    pool_share = POOL_WIDTH // N_TP
    ret_share = RET_WIDTH // N_TP
    total = jnp.zeros((SEQ, D), jnp.float32)
    for index in range(N_TP):
        part_pool = jnp.dot(pool_out[:, index * pool_share:(index + 1) * pool_share], w_out_pool[index * pool_share:(index + 1) * pool_share], preferred_element_type=jnp.float32)
        part_ret = jnp.dot(ret_out[:, index * ret_share:(index + 1) * ret_share], w_out_ret[index * ret_share:(index + 1) * ret_share], preferred_element_type=jnp.float32)
        total = total + (part_pool + part_ret).astype(jnp.bfloat16).astype(jnp.float32)
    return total.astype(jnp.bfloat16)
```

```python
import functools
import math

import jax
import jax.numpy as jnp
from jax import lax
from jax.experimental import pallas as pl
from jax.experimental.pallas import tpu as pltpu
from jax.sharding import PartitionSpec as P

GROUP_DIM = 256
HEAD_DIM = 128
CHUNK = 256
SUB = 128
RIM = 16
F32 = jnp.float32
BF16 = jnp.bfloat16


def dot(a, b):
    return jnp.dot(a, b, preferred_element_type=F32)


def layer_kernel(
    n_sp,
    n_tp,
    tokens,
    norm_gain,
    w_pool,
    w_query,
    w_key,
    w_value,
    w_gate,
    pool_mix,
    pool_bias,
    pool_gain,
    ret_gain,
    w_out_pool,
    w_out_ret,
    out,
    tok,
    wts,
    pr,
    wo,
    kr,
    qr,
    raw,
    cat,
    cosine,
    sine,
    decay,
    qdec,
    kdec,
    states,
    total,
    sin_buf,
    sout_buf,
    band,
    part_send,
    part_recv,
    out_buf,
    tok_sem,
    w_sem,
    wo_sem,
    tok_rs,
    st_send,
    st_recv,
    rim_rs,
    part_ss,
    part_rs,
    out_sem,
):
    tp = lax.axis_index("tp")
    sp = lax.axis_index("sp")
    rows = tokens.shape[0]
    length = rows * n_tp
    width = w_query.shape[1]
    wide = wo.shape[1]
    heads = width // HEAD_DIM
    groups = w_pool.shape[1] // GROUP_DIM
    chunks = length // CHUNK
    seq_len = length * n_sp
    own = pl.multiple_of(tp * rows, rows)
    other = pl.multiple_of((n_tp - 1 - tp) * rows, rows)
    peer = {"tp": n_tp - 1 - tp}

    tok_in = pltpu.make_async_copy(tokens, tok.at[pl.ds(own, rows)], tok_sem)
    tok_in.start()
    w_in = [
        pltpu.make_async_copy(w, wts.at[i], w_sem.at[i])
        for i, w in enumerate((w_key, w_value, w_pool, w_query, w_gate))
    ]
    for copy in w_in:
        copy.start()
    half = w_out_pool.shape[0]
    wo_in = [
        pltpu.make_async_copy(w_out_pool, wo.at[pl.ds(0, half)], wo_sem.at[0]),
        pltpu.make_async_copy(w_out_ret, wo.at[pl.ds(half, width)], wo_sem.at[1]),
    ]
    for copy in wo_in:
        copy.start()

    barrier = pltpu.get_barrier_semaphore()
    pl.semaphore_signal(barrier, inc=1, device_id=peer, device_id_type=pl.DeviceIdType.MESH)

    @pl.when(sp > 0)
    def _():
        pl.semaphore_signal(
            barrier, inc=1, device_id={"sp": sp - 1}, device_id_type=pl.DeviceIdType.MESH
        )

    @pl.when(sp < n_sp - 1)
    def _():
        pl.semaphore_signal(
            barrier, inc=1, device_id={"sp": sp + 1}, device_id_type=pl.DeviceIdType.MESH
        )

    neighbours = jnp.where(sp > 0, 1, 0) + jnp.where(sp < n_sp - 1, 1, 0)
    pl.semaphore_wait(barrier, 1 + neighbours)

    tok_out = pltpu.make_async_remote_copy(
        src_ref=tokens,
        dst_ref=tok.at[pl.ds(own, rows)],
        send_sem=tok_rs.at[0],
        recv_sem=tok_rs.at[1],
        device_id=peer,
        device_id_type=pl.DeviceIdType.MESH,
    )
    tok_out.start()

    def log_decay(h):
        total_heads = heads * n_tp
        value = jnp.float32(0.0)
        for t in range(n_tp):
            one = -(2.0**-5) * (seq_len / 16.0) ** (-2.0 * (t * heads + h) / (total_heads - 1))
            value = jnp.where(tp == t, jnp.float32(one), value)
        return value

    logs = [log_decay(h) for h in range(heads)]
    lane = lax.broadcasted_iota(jnp.int32, (SUB, HEAD_DIM), 1)
    row = lax.broadcasted_iota(jnp.int32, (SUB, HEAD_DIM), 0)
    hd = HEAD_DIM // 2
    low = lane < hd
    freq = jnp.exp(
        jnp.where(low, lane, lane - hd).astype(F32) * (-math.log(10000.0) / hd)
    )
    ang = row.astype(F32) * freq
    cos_r, sin_r = jnp.cos(ang), jnp.sin(ang)
    subs = length // SUB
    base_row = lax.broadcasted_iota(jnp.int32, (subs, HEAD_DIM), 0)
    base = (sp * length + base_row * SUB).astype(F32) * freq[:subs]
    cos_b, sin_b = jnp.cos(base), jnp.sin(base)
    for b in range(subs):
        cb, sb = cos_b[b : b + 1], sin_b[b : b + 1]
        cosine[b * SUB : (b + 1) * SUB] = cb * cos_r - sb * sin_r
        s = sb * cos_r + cb * sin_r
        sine[b * SUB : (b + 1) * SUB] = jnp.where(low, -s, s)

    step_i = lax.broadcasted_iota(jnp.int32, (CHUNK, HEAD_DIM), 0).astype(F32)
    di = lax.broadcasted_iota(jnp.int32, (CHUNK, CHUNK), 0) - lax.broadcasted_iota(
        jnp.int32, (CHUNK, CHUNK), 1
    )
    dpos = jnp.maximum(di, 0).astype(F32)
    for h in range(heads):
        decay[h] = jnp.where(di >= 0, jnp.exp(logs[h] * dpos), 0.0)
        qdec[h] = jnp.exp(logs[h] * (step_i + 1.0))
        kdec[h] = jnp.exp(logs[h] * (CHUNK - 1.0 - step_i))
    bi = lax.broadcasted_iota(jnp.int32, (SUB, SUB + RIM), 0)
    bj = lax.broadcasted_iota(jnp.int32, (SUB, SUB + RIM), 1)
    back = bi + RIM - bj
    windows = [jnp.left_shift(jnp.int32(2), tp * groups + g) for g in range(groups)]
    for g in range(groups):
        band[g] = jnp.where((back >= 0) & (back < windows[g]), 1.0, 0.0).astype(BF16)

    @pl.when(sp == 0)
    def _():
        pr[2, 0:RIM] = jnp.zeros((RIM, width), BF16)
        sin_buf[...] = jnp.zeros_like(sin_buf)

    def norm_rows(start):
        step = 16

        def body(i, carry):
            at = pl.ds(pl.multiple_of(start + i * step, step), step)
            x = tok[at, :].astype(F32)
            scale = lax.rsqrt(jnp.mean(x * x, axis=-1, keepdims=True) + 1e-06)
            tok[at, :] = (x * scale * norm_gain[...]).astype(BF16)
            return carry

        lax.fori_loop(0, rows // step, body, 0)

    def project(w, start):
        start = pl.multiple_of(start, CHUNK)
        res = dot(tok[pl.ds(start, CHUNK), :], wts[w])
        pr[w, pl.ds(pl.multiple_of(start + RIM, RIM), CHUNK)] = res.astype(BF16)

    per_half = rows // CHUNK

    def kv_half(start):
        def body(i, carry):
            project(i // per_half, start + (i % per_half) * CHUNK)
            return carry

        lax.fori_loop(0, 2 * per_half, body, 0)

    tok_in.wait()
    norm_rows(own)
    w_in[0].wait()
    w_in[1].wait()
    kv_half(own)
    tok_out.wait_recv()
    norm_rows(other)
    kv_half(other)

    def rotate(x, at):
        return x * cosine[at] + pltpu.roll(x, HEAD_DIM // 2, 1) * sine[at]

    for h in range(heads):
        total[h] = jnp.zeros((HEAD_DIM, HEAD_DIM), F32)
    block_decays = [jnp.exp(jnp.full((1, HEAD_DIM), logs[h] * CHUNK, F32)) for h in range(heads)]
    length_decays = [jnp.exp(jnp.full((1, HEAD_DIM), logs[h] * length, F32)) for h in range(heads)]

    def state_body(b, carry):
        at = pl.ds(pl.multiple_of(b * CHUNK, CHUNK), CHUNK)
        pat = pl.ds(pl.multiple_of(b * CHUNK + RIM, RIM), CHUNK)
        for h in range(heads):
            cols = slice(h * HEAD_DIM, (h + 1) * HEAD_DIM)
            k = rotate(pr[0, pat, cols].astype(F32), at) * HEAD_DIM**-0.5
            kr[at, cols] = k.astype(BF16)
            kd = (k * kdec[h]).astype(BF16)
            new = lax.dot_general(
                kd, pr[1, pat, cols], (((0,), (0,)), ((), ())), preferred_element_type=F32
            )
            states[b, h] = total[h]
            total[h] = total[h] * block_decays[h] + new
        return carry

    lax.fori_loop(0, chunks, state_body, 0)
    for copy in w_in[2:]:
        copy.wait()

    slots = 3 * chunks + chunks
    st_copies = [
        pltpu.make_async_remote_copy(
            src_ref=sout_buf.at[h],
            dst_ref=sin_buf.at[h],
            send_sem=st_send.at[h],
            recv_sem=st_recv.at[h],
            device_id={"sp": sp + 1},
            device_id_type=pl.DeviceIdType.MESH,
        )
        for h in range(heads)
    ]
    rim_copy = pltpu.make_async_remote_copy(
        src_ref=pr.at[2, pl.ds(length, RIM)],
        dst_ref=pr.at[2, pl.ds(0, RIM)],
        send_sem=rim_rs.at[0],
        recv_sem=rim_rs.at[1],
        device_id={"sp": sp + 1},
        device_id_type=pl.DeviceIdType.MESH,
    )

    def relay(c):
        for h in range(heads):

            @pl.when(jnp.minimum(3 * sp + h, slots - 1) == c)
            def _():
                @pl.when(sp > 0)
                def _():
                    st_copies[h].wait_recv()

                @pl.when(sp < n_sp - 1)
                def _():
                    sout_buf[h] = (
                        total[h] + length_decays[h] * sin_buf[h].astype(F32)
                    ).astype(BF16)
                    st_copies[h].start()

    def proj_body(c, carry):
        relay(c)

        @pl.when((c == chunks) & (sp < n_sp - 1))
        def _():
            rim_copy.start()

        project(2 + c // chunks, (c % chunks) * CHUNK)
        return carry

    lax.fori_loop(0, 3 * chunks, proj_body, 0)

    @pl.when(sp > 0)
    def _():
        rim_copy.wait_recv()

    def local_body(b, carry):
        relay(3 * chunks + b)
        at = pl.ds(pl.multiple_of(b * CHUNK, CHUNK), CHUNK)
        pat = pl.ds(pl.multiple_of(b * CHUNK + RIM, RIM), CHUNK)
        for h in range(heads):
            cols = slice(h * HEAD_DIM, (h + 1) * HEAD_DIM)
            q = rotate(pr[3, pat, cols].astype(F32), at).astype(BF16)
            qr[at, cols] = q
            scores = lax.dot_general(
                q, kr[at, cols], (((1,), (1,)), ((), ())), preferred_element_type=F32
            )
            scores = (scores * decay[h]).astype(BF16)
            raw[at, cols] = dot(scores, pr[1, pat, cols]) + qdec[h] * dot(
                q, states[b, h].astype(BF16)
            )
        for s in range(CHUNK // SUB):
            first = b * CHUNK + s * SUB
            here = sp * length + first + lax.broadcasted_iota(jnp.int32, (SUB, GROUP_DIM), 0)
            for g in range(groups):
                cols = slice(g * GROUP_DIM, (g + 1) * GROUP_DIM)
                span = pr[2, pl.ds(pl.multiple_of(first, SUB), SUB + RIM), cols]
                x = pr[2, pl.ds(pl.multiple_of(first + RIM, RIM), SUB), cols].astype(F32)
                count = jnp.minimum(here + 1, windows[g]).astype(F32)
                diff = (dot(band[g], span) / count - x).astype(BF16)
                mixed = dot(diff, pool_mix[g]) + pool_bias[g : g + 1]
                cat[pl.ds(pl.multiple_of(first, SUB), SUB), cols] = (
                    mixed * pool_gain[:, cols]
                ).astype(BF16)
        return carry

    lax.fori_loop(0, chunks, local_body, 0)
    for copy in wo_in:
        copy.wait()

    def finish(start):
        at = pl.ds(pl.multiple_of(start, CHUNK), CHUNK)
        pat = pl.ds(pl.multiple_of(start + RIM, RIM), CHUNK)
        for h in range(heads):
            cols = slice(h * HEAD_DIM, (h + 1) * HEAD_DIM)
            ahead = jnp.exp(jnp.full((1, HEAD_DIM), logs[h], F32) * start.astype(F32))
            state = (sin_buf[h].astype(F32) * ahead).astype(BF16)
            r = raw[at, cols] + qdec[h] * dot(qr[at, cols], state)
            r = r - jnp.mean(r, axis=-1, keepdims=True)
            var = jnp.mean(r * r, axis=-1, keepdims=True)
            gate = pr[4, pat, cols].astype(F32)
            gated = gate * (1.0 / (1.0 + jnp.exp(-gate))) * ret_gain[:, cols]
            cat[at, half + h * HEAD_DIM : half + (h + 1) * HEAD_DIM] = (
                gated * (r * lax.rsqrt(var + 1e-06))
            ).astype(BF16)
        return at

    def part_copy(j):
        at = pl.ds(pl.multiple_of(j * CHUNK, CHUNK), CHUNK)
        return pltpu.make_async_remote_copy(
            src_ref=part_send.at[at],
            dst_ref=part_recv.at[at],
            send_sem=part_ss.at[j],
            recv_sem=part_rs.at[j],
            device_id=peer,
            device_id_type=pl.DeviceIdType.MESH,
        )

    def out_copy(j):
        at = pl.ds(pl.multiple_of(j * CHUNK, CHUNK), CHUNK)
        return pltpu.make_async_copy(out_buf.at[at], out.at[at], out_sem.at[j])

    tile = 512

    def send_body(j, carry):
        at = finish(other + j * CHUNK)
        mine = pl.ds(pl.multiple_of(j * CHUNK, CHUNK), CHUNK)
        for n in range(wide // tile):
            cols = slice(n * tile, (n + 1) * tile)
            part_send[mine, cols] = dot(cat[at, :], wo[:, cols]).astype(BF16)
        part_copy(j).start()
        return carry

    lax.fori_loop(0, per_half, send_body, 0)

    def own_body(j, carry):
        at = finish(own + j * CHUNK)
        mine = pl.ds(pl.multiple_of(j * CHUNK, CHUNK), CHUNK)
        part_copy(j).wait_recv()
        for n in range(wide // tile):
            cols = slice(n * tile, (n + 1) * tile)
            part = dot(cat[at, :], wo[:, cols]).astype(BF16).astype(F32)
            out_buf[mine, cols] = (part + part_recv[mine, cols].astype(F32)).astype(BF16)
        out_copy(j).start()
        return carry

    lax.fori_loop(0, per_half, own_body, 0)

    tok_out.wait_send()
    for j in range(per_half):
        part_copy(j).wait_send()
        out_copy(j).wait()

    @pl.when(sp < n_sp - 1)
    def _():
        rim_copy.wait_send()
        for h in range(heads):
            st_copies[h].wait_send()


def per_device(
    tokens,
    norm_gain,
    w_pool,
    w_query,
    w_key,
    w_value,
    w_gate,
    pool_mix,
    pool_bias,
    pool_gain,
    ret_gain,
    w_out_pool,
    w_out_ret,
):
    n_sp, n_tp = lax.axis_size("sp"), lax.axis_size("tp")
    rows, model = tokens.shape
    length = rows * n_tp
    width = w_query.shape[1]
    heads = width // HEAD_DIM
    pool_width = w_pool.shape[1]
    groups = pool_width // GROUP_DIM
    chunks = length // CHUNK
    per_half = rows // CHUNK
    wide = w_out_pool.shape[1]
    hbm = pl.BlockSpec(memory_space=pl.ANY)
    vmem = pl.BlockSpec(memory_space=pltpu.VMEM)
    dma = pltpu.SemaphoreType.DMA
    flops = 2 * length * model * (pool_width + 4 * width) + 2 * length * (pool_width + width) * wide
    return pl.pallas_call(
        functools.partial(layer_kernel, n_sp, n_tp),
        out_shape=jax.ShapeDtypeStruct((rows, wide), BF16),
        in_specs=[hbm, vmem, hbm, hbm, hbm, hbm, hbm, vmem, vmem, vmem, vmem, hbm, hbm],
        out_specs=hbm,
        scratch_shapes=[
            pltpu.VMEM((length, model), BF16),
            pltpu.VMEM((5, model, width), BF16),
            pltpu.VMEM((5, length + RIM, width), BF16),
            pltpu.VMEM((pool_width + width, wide), BF16),
            pltpu.VMEM((length, width), BF16),
            pltpu.VMEM((length, width), BF16),
            pltpu.VMEM((length, width), F32),
            pltpu.VMEM((length, pool_width + width), BF16),
            pltpu.VMEM((length, HEAD_DIM), F32),
            pltpu.VMEM((length, HEAD_DIM), F32),
            pltpu.VMEM((heads, CHUNK, CHUNK), F32),
            pltpu.VMEM((heads, CHUNK, HEAD_DIM), F32),
            pltpu.VMEM((heads, CHUNK, HEAD_DIM), F32),
            pltpu.VMEM((chunks, heads, HEAD_DIM, HEAD_DIM), F32),
            pltpu.VMEM((heads, HEAD_DIM, HEAD_DIM), F32),
            pltpu.VMEM((heads, HEAD_DIM, HEAD_DIM), BF16),
            pltpu.VMEM((heads, HEAD_DIM, HEAD_DIM), BF16),
            pltpu.VMEM((groups, SUB, SUB + RIM), BF16),
            pltpu.VMEM((rows, wide), BF16),
            pltpu.VMEM((rows, wide), BF16),
            pltpu.VMEM((rows, wide), BF16),
            dma,
            dma((5,)),
            dma((2,)),
            dma((2,)),
            dma((heads,)),
            dma((heads,)),
            dma((2,)),
            dma((per_half,)),
            dma((per_half,)),
            dma((per_half,)),
        ],
        compiler_params=pltpu.CompilerParams(
            collective_id=0, has_side_effects=True, vmem_limit_bytes=62 * 1024 * 1024
        ),
        cost_estimate=pl.CostEstimate(
            flops=flops, bytes_accessed=20 * 1024 * 1024, transcendentals=0
        ),
    )(
        tokens,
        norm_gain.reshape(1, -1),
        w_pool,
        w_query,
        w_key,
        w_value,
        w_gate,
        pool_mix,
        pool_bias,
        pool_gain.reshape(1, -1),
        ret_gain.reshape(1, -1),
        w_out_pool,
        w_out_ret,
    )


def solution(mesh):
    return jax.shard_map(
        per_device,
        mesh=mesh,
        in_specs=(
            P(("fs", "sp", "tp"), None),
            P(),
            P(None, "tp"),
            P(None, "tp"),
            P(None, "tp"),
            P(None, "tp"),
            P(None, "tp"),
            P("tp", None, None),
            P("tp", None),
            P("tp"),
            P("tp"),
            P("tp", None),
            P("tp", None),
        ),
        out_specs=P(("fs", "sp", "tp"), None),
        check_vma=False,
    )
```

```python
import functools
import math

import jax
import jax.numpy as jnp
from jax import lax
from jax.experimental import pallas as pl
from jax.experimental.pallas import tpu as pltpu
from jax.sharding import PartitionSpec as P

GROUP_DIM = 256
HEAD_DIM = 128
CHUNK = 256
SUB = 128
RIM = 16
HOP = 4
F32 = jnp.float32
BF16 = jnp.bfloat16


def dot(a, b):
    return jnp.dot(a, b, preferred_element_type=F32)


def layer_kernel(
    n_sp,
    n_tp,
    tokens,
    norm_gain,
    w_pool,
    w_query,
    w_key,
    w_value,
    w_gate,
    pool_mix,
    pool_bias,
    pool_gain,
    ret_gain,
    w_out_pool,
    w_out_ret,
    out_own,
    part_recv,
    tok,
    wts,
    pk,
    pv,
    pp,
    pq,
    pg,
    wo,
    kr,
    qr,
    raw,
    pool_out,
    ret_a,
    ret_b,
    cosine,
    sine,
    decay,
    qdec,
    kdec,
    states,
    total,
    sin_buf,
    sout_buf,
    band,
    ldec,
    part_send,
    tok_sem,
    w_sem,
    wo_sem,
    tok_rs,
    st_send,
    st_recv,
    rim_rs,
    part_ss,
    part_rs,
):
    tp = lax.axis_index("tp")
    sp = lax.axis_index("sp")
    rows = tokens.shape[0]
    length = rows * n_tp
    width = w_query.shape[1]
    wide = wo.shape[1]
    heads = width // HEAD_DIM
    groups = w_pool.shape[1] // GROUP_DIM
    chunks = length // CHUNK
    seq_len = length * n_sp
    own = pl.multiple_of(tp * rows, rows)
    other = pl.multiple_of((n_tp - 1 - tp) * rows, rows)
    peer = {"tp": n_tp - 1 - tp}

    tok_in = pltpu.make_async_copy(tokens, tok.at[pl.ds(own, rows)], tok_sem)
    tok_in.start()
    w_in = [
        pltpu.make_async_copy(w, wts.at[i], w_sem.at[i])
        for i, w in enumerate((w_key, w_value, w_pool, w_query, w_gate))
    ]
    w_in[0].start()
    w_in[1].start()
    half = w_out_pool.shape[0]
    wo_in = [
        pltpu.make_async_copy(w_out_pool, wo.at[pl.ds(0, half)], wo_sem.at[0]),
        pltpu.make_async_copy(w_out_ret, wo.at[pl.ds(half, width)], wo_sem.at[1]),
    ]

    barrier = pltpu.get_barrier_semaphore()
    pl.semaphore_signal(barrier, inc=1, device_id=peer, device_id_type=pl.DeviceIdType.MESH)

    @pl.when(sp > 0)
    def _():
        pl.semaphore_signal(
            barrier, inc=1, device_id={"sp": sp - 1}, device_id_type=pl.DeviceIdType.MESH
        )

    @pl.when(sp < n_sp - 1)
    def _():
        pl.semaphore_signal(
            barrier, inc=1, device_id={"sp": sp + 1}, device_id_type=pl.DeviceIdType.MESH
        )

    def log_decay(h):
        total_heads = heads * n_tp
        value = jnp.float32(0.0)
        for t in range(n_tp):
            one = -(2.0**-5) * (seq_len / 16.0) ** (-2.0 * (t * heads + h) / (total_heads - 1))
            value = jnp.where(tp == t, jnp.float32(one), value)
        return value

    logs = [log_decay(h) for h in range(heads)]
    lane = lax.broadcasted_iota(jnp.int32, (SUB, HEAD_DIM), 1)
    row = lax.broadcasted_iota(jnp.int32, (SUB, HEAD_DIM), 0)
    hd = HEAD_DIM // 2
    low = lane < hd
    freq = jnp.exp(
        jnp.where(low, lane, lane - hd).astype(F32) * (-math.log(10000.0) / hd)
    )
    ang = row.astype(F32) * freq
    cos_r, sin_r = jnp.cos(ang), jnp.sin(ang)
    subs = length // SUB
    base_row = lax.broadcasted_iota(jnp.int32, (subs, HEAD_DIM), 0)
    base = (sp * length + base_row * SUB).astype(F32) * freq[:subs]
    cos_b, sin_b = jnp.cos(base), jnp.sin(base)
    for b in range(subs):
        cb, sb = cos_b[b : b + 1], sin_b[b : b + 1]
        cosine[b * SUB : (b + 1) * SUB] = cb * cos_r - sb * sin_r
        s = sb * cos_r + cb * sin_r
        sine[b * SUB : (b + 1) * SUB] = jnp.where(low, -s, s)

    step_i = lax.broadcasted_iota(jnp.int32, (CHUNK, HEAD_DIM), 0).astype(F32)
    di = lax.broadcasted_iota(jnp.int32, (CHUNK, CHUNK), 0) - lax.broadcasted_iota(
        jnp.int32, (CHUNK, CHUNK), 1
    )
    dpos = jnp.maximum(di, 0).astype(F32)
    for h in range(heads):
        decay[h] = jnp.where(di >= 0, jnp.exp(logs[h] * dpos), 0.0)
        qdec[h] = jnp.exp(logs[h] * (step_i + 1.0))
        kdec[h] = jnp.exp(logs[h] * (CHUNK - 1.0 - step_i))
    bi = lax.broadcasted_iota(jnp.int32, (SUB, SUB + RIM), 0)
    bj = lax.broadcasted_iota(jnp.int32, (SUB, SUB + RIM), 1)
    back = bi + RIM - bj
    windows = [jnp.left_shift(jnp.int32(2), tp * groups + g) for g in range(groups)]
    for g in range(groups):
        band[g] = jnp.where((back >= 0) & (back < windows[g]), 1.0, 0.0).astype(BF16)

    @pl.when(sp == 0)
    def _():
        pp[0:RIM] = jnp.zeros((RIM, width), BF16)
        sin_buf[...] = jnp.zeros_like(sin_buf)

    neighbours = jnp.where(sp > 0, 1, 0) + jnp.where(sp < n_sp - 1, 1, 0)
    pl.semaphore_wait(barrier, 1 + neighbours)

    tok_out = pltpu.make_async_remote_copy(
        src_ref=tokens,
        dst_ref=tok.at[pl.ds(own, rows)],
        send_sem=tok_rs.at[0],
        recv_sem=tok_rs.at[1],
        device_id=peer,
        device_id_type=pl.DeviceIdType.MESH,
    )
    tok_out.start()

    def norm_rows(start):
        step = 16

        def body(i, carry):
            at = pl.ds(pl.multiple_of(start + i * step, step), step)
            x = tok[at, :].astype(F32)
            scale = lax.rsqrt(jnp.mean(x * x, axis=-1, keepdims=True) + 1e-06)
            tok[at, :] = (x * scale * norm_gain[...]).astype(BF16)
            return carry

        lax.fori_loop(0, rows // step, body, 0, unroll=4)

    def project(w, dst, start, pad=0):
        start = pl.multiple_of(start, CHUNK)
        res = dot(tok[pl.ds(start, CHUNK), :], wts[w])
        dst[pl.ds(pl.multiple_of(start + pad, RIM), CHUNK)] = res.astype(BF16)

    per_half = rows // CHUNK

    def kv_half(start):
        def body(i, carry):
            project(0, pk, start + i * CHUNK)
            project(1, pv, start + i * CHUNK)
            return carry

        lax.fori_loop(0, per_half, body, 0)

    tok_in.wait()
    for copy in w_in[2:] + wo_in:
        copy.start()
    norm_rows(own)
    w_in[0].wait()
    w_in[1].wait()
    kv_half(own)
    tok_out.wait_recv()
    norm_rows(other)
    kv_half(other)

    def rotate(x, at):
        return x * cosine[at] + pltpu.roll(x, HEAD_DIM // 2, 1) * sine[at]

    for h in range(heads):
        total[h] = jnp.zeros((HEAD_DIM, HEAD_DIM), F32)
    block_decays = [jnp.exp(jnp.full((1, HEAD_DIM), logs[h] * CHUNK, F32)) for h in range(heads)]
    for h in range(heads):
        ldec[h] = jnp.exp(jnp.full((8, HEAD_DIM), logs[h] * length, F32))

    def state_body(b, carry):
        at = pl.ds(pl.multiple_of(b * CHUNK, CHUNK), CHUNK)
        for h in range(heads):
            cols = slice(h * HEAD_DIM, (h + 1) * HEAD_DIM)
            k = rotate(pk[at, cols].astype(F32), at) * HEAD_DIM**-0.5
            kr[at, cols] = k.astype(BF16)
            kd = (k * kdec[h]).astype(BF16)
            new = lax.dot_general(
                kd, pv[at, cols], (((0,), (0,)), ((), ())), preferred_element_type=F32
            )
            states[b, h] = total[h]
            total[h] = total[h] * block_decays[h] + new
        return carry

    lax.fori_loop(0, chunks, state_body, 0)
    for copy in w_in[2:]:
        copy.wait()

    slots = 3 * chunks

    def st_copy(h):
        return pltpu.make_async_remote_copy(
            src_ref=sout_buf.at[h],
            dst_ref=sin_buf.at[h],
            send_sem=st_send.at[h],
            recv_sem=st_recv.at[h],
            device_id={"sp": sp + 1},
            device_id_type=pl.DeviceIdType.MESH,
        )

    rim_copy = pltpu.make_async_remote_copy(
        src_ref=pp.at[pl.ds(length, RIM)],
        dst_ref=pp.at[pl.ds(0, RIM)],
        send_sem=rim_rs.at[0],
        recv_sem=rim_rs.at[1],
        device_id={"sp": sp + 1},
        device_id_type=pl.DeviceIdType.MESH,
    )

    def relay_head(h):
        @pl.when(sp > 0)
        def _():
            st_copy(h).wait_recv()

        @pl.when(sp < n_sp - 1)
        def _():
            sout_buf[h] = (total[h] + ldec[h, 0:1] * sin_buf[h].astype(F32)).astype(BF16)
            st_copy(h).start()

    def relay(c):
        h = c - HOP * sp

        @pl.when((h >= 0) & (h < heads) & (sp > 0))
        def _():
            relay_head(h)

    @pl.when(sp == 0)
    def _():
        for h in range(heads):
            relay_head(h)

    def pool_body(c, carry):
        relay(c)
        project(2, pp, c * CHUNK, RIM)
        return carry

    lax.fori_loop(0, chunks, pool_body, 0)

    def query_body(c, carry):
        relay(chunks + c)

        @pl.when((c == 1) & (sp < n_sp - 1))
        def _():
            rim_copy.start()

        project(3, pq, c * CHUNK)
        return carry

    lax.fori_loop(0, chunks, query_body, 0)

    @pl.when(sp > 0)
    def _():
        rim_copy.wait_recv()

    def local_body(b, carry):
        relay(2 * chunks + b)
        project(4, pg, b * CHUNK)
        at = pl.ds(pl.multiple_of(b * CHUNK, CHUNK), CHUNK)
        for h in range(heads):
            cols = slice(h * HEAD_DIM, (h + 1) * HEAD_DIM)
            q = rotate(pq[at, cols].astype(F32), at).astype(BF16)
            qr[at, cols] = q
            scores = lax.dot_general(
                q, kr[at, cols], (((1,), (1,)), ((), ())), preferred_element_type=F32
            )
            scores = (scores * decay[h]).astype(BF16)
            raw[at, cols] = dot(scores, pv[at, cols]) + qdec[h] * dot(
                q, states[b, h].astype(BF16)
            )
        for s in range(CHUNK // SUB):
            first = b * CHUNK + s * SUB
            here = sp * length + first + lax.broadcasted_iota(jnp.int32, (SUB, GROUP_DIM), 0)
            for g in range(groups):
                cols = slice(g * GROUP_DIM, (g + 1) * GROUP_DIM)
                span = pp[pl.ds(pl.multiple_of(first, SUB), SUB + RIM), cols]
                x = pp[pl.ds(pl.multiple_of(first + RIM, RIM), SUB), cols].astype(F32)
                count = jnp.minimum(here + 1, windows[g]).astype(F32)
                diff = (dot(band[g], span) / count - x).astype(BF16)
                mixed = dot(diff, pool_mix[g]) + pool_bias[g : g + 1]
                pool_out[pl.ds(pl.multiple_of(first, SUB), SUB), cols] = (
                    mixed * pool_gain[:, cols]
                ).astype(BF16)
        return carry

    lax.fori_loop(0, chunks, local_body, 0)

    def rest(h, carry):
        @pl.when((h + HOP * sp >= slots) & (sp > 0))
        def _():
            relay_head(h)

        return carry

    lax.fori_loop(0, heads, rest, 0)
    for copy in wo_in:
        copy.wait()

    def finish(start, ret):
        at = pl.ds(pl.multiple_of(start, CHUNK), CHUNK)
        for h in range(heads):
            cols = slice(h * HEAD_DIM, (h + 1) * HEAD_DIM)
            ahead = jnp.exp(jnp.full((1, HEAD_DIM), logs[h], F32) * start.astype(F32))
            state = (sin_buf[h].astype(F32) * ahead).astype(BF16)
            r = raw[at, cols] + qdec[h] * dot(qr[at, cols], state)
            r = r - jnp.mean(r, axis=-1, keepdims=True)
            var = jnp.mean(r * r, axis=-1, keepdims=True)
            gate = pg[at, cols].astype(F32)
            gated = gate * (1.0 / (1.0 + jnp.exp(-gate))) * ret_gain[:, cols]
            ret[:, cols] = (
                gated * (r * lax.rsqrt(var + 1e-06))
            ).astype(BF16)

    def part_copy(j):
        at = pl.ds(pl.multiple_of(j * CHUNK, CHUNK), CHUNK)
        return pltpu.make_async_remote_copy(
            src_ref=part_send.at[at],
            dst_ref=part_recv.at[at],
            send_sem=part_ss.at[j],
            recv_sem=part_rs.at[j],
            device_id=peer,
            device_id_type=pl.DeviceIdType.MESH,
        )

    tile = 512

    def multiply(start, ret, dst, j):
        at = pl.ds(pl.multiple_of(start, CHUNK), CHUNK)
        mine = slice(j * CHUNK, (j + 1) * CHUNK)
        left = jnp.concatenate([pool_out[at, :], ret[...]], axis=1)
        for n in range(wide // tile):
            cols = slice(n * tile, (n + 1) * tile)
            dst[mine, cols] = dot(left, wo[:, cols]).astype(BF16)

    starts = [other + j * CHUNK for j in range(per_half)] + [
        own + j * CHUNK for j in range(per_half)
    ]
    rets = (ret_a, ret_b)
    finish(starts[0], ret_a)
    for i, start in enumerate(starts):
        sending = i < per_half
        multiply(start, rets[i % 2], part_send if sending else out_own, i % per_half)
        if i + 1 < len(starts):
            finish(starts[i + 1], rets[(i + 1) % 2])
        if sending:
            part_copy(i).start()

    for j in range(per_half):
        part_copy(j).wait_recv()

    tok_out.wait_send()
    for j in range(per_half):
        part_copy(j).wait_send()

    @pl.when(sp < n_sp - 1)
    def _():
        rim_copy.wait_send()
        for h in range(heads):
            st_copy(h).wait_send()


def per_device(
    tokens,
    norm_gain,
    w_pool,
    w_query,
    w_key,
    w_value,
    w_gate,
    pool_mix,
    pool_bias,
    pool_gain,
    ret_gain,
    w_out_pool,
    w_out_ret,
):
    n_sp, n_tp = lax.axis_size("sp"), lax.axis_size("tp")
    rows, model = tokens.shape
    length = rows * n_tp
    width = w_query.shape[1]
    heads = width // HEAD_DIM
    pool_width = w_pool.shape[1]
    groups = pool_width // GROUP_DIM
    chunks = length // CHUNK
    per_half = rows // CHUNK
    wide = w_out_pool.shape[1]
    hbm = pl.BlockSpec(memory_space=pltpu.HBM)
    vmem = pl.BlockSpec(memory_space=pltpu.VMEM)
    dma = pltpu.SemaphoreType.DMA
    flops = 2 * length * model * (pool_width + 4 * width) + 2 * length * (pool_width + width) * wide
    own, received = pl.pallas_call(
        functools.partial(layer_kernel, n_sp, n_tp),
        out_shape=[pltpu.VMEM((rows, wide), BF16)] * 2,
        in_specs=[hbm, vmem, hbm, hbm, hbm, hbm, hbm, vmem, vmem, vmem, vmem, hbm, hbm],
        out_specs=[vmem, vmem],
        scratch_shapes=[
            pltpu.VMEM((length, model), BF16),
            pltpu.VMEM((5, model, width), BF16),
            pltpu.VMEM((length, width), BF16),
            pltpu.VMEM((length, width), BF16),
            pltpu.VMEM((length + RIM, pool_width), BF16),
            pltpu.VMEM((length, width), BF16),
            pltpu.VMEM((length, width), BF16),
            pltpu.VMEM((pool_width + width, wide), BF16),
            pltpu.VMEM((length, width), BF16),
            pltpu.VMEM((length, width), BF16),
            pltpu.VMEM((length, width), F32),
            pltpu.VMEM((length, pool_width), BF16),
            pltpu.VMEM((CHUNK, width), BF16),
            pltpu.VMEM((CHUNK, width), BF16),
            pltpu.VMEM((length, HEAD_DIM), F32),
            pltpu.VMEM((length, HEAD_DIM), F32),
            pltpu.VMEM((heads, CHUNK, CHUNK), F32),
            pltpu.VMEM((heads, CHUNK, HEAD_DIM), F32),
            pltpu.VMEM((heads, CHUNK, HEAD_DIM), F32),
            pltpu.VMEM((chunks, heads, HEAD_DIM, HEAD_DIM), F32),
            pltpu.VMEM((heads, HEAD_DIM, HEAD_DIM), F32),
            pltpu.VMEM((heads, HEAD_DIM, HEAD_DIM), BF16),
            pltpu.VMEM((heads, HEAD_DIM, HEAD_DIM), BF16),
            pltpu.VMEM((groups, SUB, SUB + RIM), BF16),
            pltpu.VMEM((heads, 8, HEAD_DIM), F32),
            pltpu.VMEM((rows, wide), BF16),
            dma,
            dma((5,)),
            dma((2,)),
            dma((2,)),
            dma((heads,)),
            dma((heads,)),
            dma((2,)),
            dma((per_half,)),
            dma((per_half,)),
        ],
        compiler_params=pltpu.CompilerParams(
            collective_id=0, has_side_effects=True, vmem_limit_bytes=50 * 1024 * 1024
        ),
        cost_estimate=pl.CostEstimate(
            flops=flops, bytes_accessed=20 * 1024 * 1024, transcendentals=0
        ),
    )(
        tokens,
        norm_gain.reshape(1, -1),
        w_pool,
        w_query,
        w_key,
        w_value,
        w_gate,
        pool_mix,
        pool_bias,
        pool_gain.reshape(1, -1),
        ret_gain.reshape(1, -1),
        w_out_pool,
        w_out_ret,
    )
    return (own.astype(F32) + received.astype(F32)).astype(BF16)


def solution(mesh):
    return jax.shard_map(
        per_device,
        mesh=mesh,
        in_specs=(
            P(("fs", "sp", "tp"), None),
            P(),
            P(None, "tp"),
            P(None, "tp"),
            P(None, "tp"),
            P(None, "tp"),
            P(None, "tp"),
            P("tp", None, None),
            P("tp", None),
            P("tp"),
            P("tp"),
            P("tp", None),
            P("tp", None),
        ),
        out_specs=P(("fs", "sp", "tp"), None),
        check_vma=False,
    )
```

```python
import functools
import math

import jax
import jax.numpy as jnp
from jax import lax
from jax.experimental import pallas as pl
from jax.experimental.pallas import tpu as pltpu
from jax.sharding import PartitionSpec as P

GROUP_DIM = 256
HEAD_DIM = 128
CHUNK = 256
SUB = 128
RIM = 16
HOP = 2
PARTS = 4
F32 = jnp.float32
BF16 = jnp.bfloat16


def dot(a, b):
    return jnp.dot(a, b, preferred_element_type=F32)


def layer_kernel(
    n_sp,
    n_tp,
    tokens,
    norm_gain,
    w_pool,
    w_query,
    w_key,
    w_value,
    w_gate,
    pool_mix,
    pool_bias,
    pool_gain,
    ret_gain,
    w_out_pool,
    w_out_ret,
    out_own,
    part_recv,
    tok,
    wts,
    pk,
    pv,
    pp,
    pq,
    pg,
    wo,
    kr,
    qr,
    raw,
    pool_out,
    ret_a,
    ret_b,
    cosine,
    sine,
    decay,
    qdec,
    kdec,
    states,
    total,
    sin_buf,
    sout_buf,
    band,
    ldec,
    part_send,
    tok_sem,
    w_sem,
    wo_sem,
    tok_ss,
    tok_rs,
    st_send,
    st_recv,
    rim_rs,
    part_ss,
    part_rs,
):
    tp = lax.axis_index("tp")
    sp = lax.axis_index("sp")
    rows = tokens.shape[0]
    length = rows * n_tp
    width = w_query.shape[1]
    wide = wo.shape[1]
    heads = width // HEAD_DIM
    groups = w_pool.shape[1] // GROUP_DIM
    chunks = length // CHUNK
    seq_len = length * n_sp
    own = pl.multiple_of(tp * rows, rows)
    other = pl.multiple_of((n_tp - 1 - tp) * rows, rows)
    peer = {"tp": n_tp - 1 - tp}

    tok_in = pltpu.make_async_copy(tokens, tok.at[pl.ds(own, rows)], tok_sem)
    tok_in.start()
    w_in = [
        pltpu.make_async_copy(w, wts.at[i], w_sem.at[i])
        for i, w in enumerate((w_key, w_value, w_pool, w_query, w_gate))
    ]
    w_in[0].start()
    w_in[1].start()
    half = w_out_pool.shape[0]
    wo_in = [
        pltpu.make_async_copy(w_out_pool, wo.at[pl.ds(0, half)], wo_sem.at[0]),
        pltpu.make_async_copy(w_out_ret, wo.at[pl.ds(half, width)], wo_sem.at[1]),
    ]

    barrier = pltpu.get_barrier_semaphore()
    pl.semaphore_signal(barrier, inc=1, device_id=peer, device_id_type=pl.DeviceIdType.MESH)

    @pl.when(sp > 0)
    def _():
        pl.semaphore_signal(
            barrier, inc=1, device_id={"sp": sp - 1}, device_id_type=pl.DeviceIdType.MESH
        )

    @pl.when(sp < n_sp - 1)
    def _():
        pl.semaphore_signal(
            barrier, inc=1, device_id={"sp": sp + 1}, device_id_type=pl.DeviceIdType.MESH
        )

    def log_decay(h):
        total_heads = heads * n_tp
        value = jnp.float32(0.0)
        for t in range(n_tp):
            one = -(2.0**-5) * (seq_len / 16.0) ** (-2.0 * (t * heads + h) / (total_heads - 1))
            value = jnp.where(tp == t, jnp.float32(one), value)
        return value

    logs = [log_decay(h) for h in range(heads)]
    lane = lax.broadcasted_iota(jnp.int32, (SUB, HEAD_DIM), 1)
    row = lax.broadcasted_iota(jnp.int32, (SUB, HEAD_DIM), 0)
    hd = HEAD_DIM // 2
    low = lane < hd
    freq = jnp.exp(
        jnp.where(low, lane, lane - hd).astype(F32) * (-math.log(10000.0) / hd)
    )
    ang = row.astype(F32) * freq
    cos_r, sin_r = jnp.cos(ang), jnp.sin(ang)
    subs = length // SUB
    base_row = lax.broadcasted_iota(jnp.int32, (subs, HEAD_DIM), 0)
    base = (sp * length + base_row * SUB).astype(F32) * freq[:subs]
    cos_b, sin_b = jnp.cos(base), jnp.sin(base)
    for b in range(subs):
        cb, sb = cos_b[b : b + 1], sin_b[b : b + 1]
        cosine[b * SUB : (b + 1) * SUB] = cb * cos_r - sb * sin_r
        s = sb * cos_r + cb * sin_r
        sine[b * SUB : (b + 1) * SUB] = jnp.where(low, -s, s)

    step_i = lax.broadcasted_iota(jnp.int32, (CHUNK, HEAD_DIM), 0).astype(F32)
    di = lax.broadcasted_iota(jnp.int32, (CHUNK, CHUNK), 0) - lax.broadcasted_iota(
        jnp.int32, (CHUNK, CHUNK), 1
    )
    dpos = jnp.maximum(di, 0).astype(F32)
    for h in range(heads):
        decay[h] = jnp.where(di >= 0, jnp.exp(logs[h] * dpos), 0.0)
        qdec[h] = jnp.exp(logs[h] * (step_i + 1.0))
        kdec[h] = jnp.exp(logs[h] * (CHUNK - 1.0 - step_i))
    bi = lax.broadcasted_iota(jnp.int32, (SUB, SUB + RIM), 0)
    bj = lax.broadcasted_iota(jnp.int32, (SUB, SUB + RIM), 1)
    back = bi + RIM - bj
    windows = [jnp.left_shift(jnp.int32(2), tp * groups + g) for g in range(groups)]
    for g in range(groups):
        band[g] = jnp.where((back >= 0) & (back < windows[g]), 1.0, 0.0).astype(BF16)

    @pl.when(sp == 0)
    def _():
        pp[0:RIM] = jnp.zeros((RIM, width), BF16)
        sin_buf[...] = jnp.zeros_like(sin_buf)

    neighbours = jnp.where(sp > 0, 1, 0) + jnp.where(sp < n_sp - 1, 1, 0)
    pl.semaphore_wait(barrier, 1 + neighbours)

    part = rows // PARTS

    def tok_copy(i):
        at = pl.ds(pl.multiple_of(own + i * part, part), part)
        return pltpu.make_async_remote_copy(
            src_ref=tok.at[at],
            dst_ref=tok.at[at],
            send_sem=tok_ss.at[i],
            recv_sem=tok_rs.at[i],
            device_id=peer,
            device_id_type=pl.DeviceIdType.MESH,
        )

    def norm_rows(start):
        step = 16

        def body(i, carry):
            at = pl.ds(pl.multiple_of(start + i * step, step), step)
            x = tok[at, :].astype(F32)
            scale = lax.rsqrt(jnp.mean(x * x, axis=-1, keepdims=True) + 1e-06)
            tok[at, :] = (x * scale * norm_gain[...]).astype(BF16)
            return carry

        lax.fori_loop(0, part // step, body, 0, unroll=4)

    def project(w, dst, start, pad=0):
        start = pl.multiple_of(start, CHUNK)
        res = dot(tok[pl.ds(start, CHUNK), :], wts[w])
        dst[pl.ds(pl.multiple_of(start + pad, RIM), CHUNK)] = res.astype(BF16)

    per_half = rows // CHUNK

    def kv_half(start):
        def body(i, carry):
            project(0, pk, start + i * CHUNK)
            project(1, pv, start + i * CHUNK)
            return carry

        lax.fori_loop(0, per_half, body, 0)

    tok_in.wait()
    for copy in w_in[2:] + wo_in:
        copy.start()
    for i in range(PARTS):
        norm_rows(own + i * part)
        if i > 0:
            tok_copy(i - 1).start()
    w_in[0].wait()
    w_in[1].wait()
    tok_copy(PARTS - 1).start()
    kv_half(own)
    for i in range(PARTS):
        tok_copy(i).wait_recv()
    kv_half(other)

    def rotate(x, at):
        return x * cosine[at] + pltpu.roll(x, HEAD_DIM // 2, 1) * sine[at]

    for h in range(heads):
        total[h] = jnp.zeros((HEAD_DIM, HEAD_DIM), F32)
    block_decays = [jnp.exp(jnp.full((1, HEAD_DIM), logs[h] * CHUNK, F32)) for h in range(heads)]
    for h in range(heads):
        ldec[h] = jnp.exp(jnp.full((8, HEAD_DIM), logs[h] * length, F32))

    def state_body(b, carry):
        at = pl.ds(pl.multiple_of(b * CHUNK, CHUNK), CHUNK)
        for h in range(heads):
            cols = slice(h * HEAD_DIM, (h + 1) * HEAD_DIM)
            k = rotate(pk[at, cols].astype(F32), at) * HEAD_DIM**-0.5
            kr[at, cols] = k.astype(BF16)
            kd = (k * kdec[h]).astype(BF16)
            new = lax.dot_general(
                kd, pv[at, cols], (((0,), (0,)), ((), ())), preferred_element_type=F32
            )
            states[b, h] = total[h]
            total[h] = total[h] * block_decays[h] + new
        return carry

    lax.fori_loop(0, chunks, state_body, 0)
    for copy in w_in[2:]:
        copy.wait()

    slots = 3 * chunks

    def st_copy(h):
        return pltpu.make_async_remote_copy(
            src_ref=sout_buf.at[h],
            dst_ref=sin_buf.at[h],
            send_sem=st_send.at[h],
            recv_sem=st_recv.at[h],
            device_id={"sp": sp + 1},
            device_id_type=pl.DeviceIdType.MESH,
        )

    rim_copy = pltpu.make_async_remote_copy(
        src_ref=pp.at[pl.ds(length, RIM)],
        dst_ref=pp.at[pl.ds(0, RIM)],
        send_sem=rim_rs.at[0],
        recv_sem=rim_rs.at[1],
        device_id={"sp": sp + 1},
        device_id_type=pl.DeviceIdType.MESH,
    )

    def relay_head(h):
        @pl.when(sp > 0)
        def _():
            st_copy(h).wait_recv()

        @pl.when(sp < n_sp - 1)
        def _():
            sout_buf[h] = (total[h] + ldec[h, 0:1] * sin_buf[h].astype(F32)).astype(BF16)
            st_copy(h).start()

    def relay(c):
        h = c - HOP * sp

        @pl.when((h >= 0) & (h < heads) & (sp > 0) & (sp < n_sp - 1))
        def _():
            relay_head(h)

    @pl.when(sp == 0)
    def _():
        for h in range(heads):
            relay_head(h)

    def pool_body(c, carry):
        relay(c)
        project(2, pp, c * CHUNK, RIM)
        return carry

    lax.fori_loop(0, chunks, pool_body, 0)

    def query_body(c, carry):
        relay(chunks + c)

        @pl.when((c == 1) & (sp < n_sp - 1))
        def _():
            rim_copy.start()

        project(3, pq, c * CHUNK)
        return carry

    lax.fori_loop(0, chunks, query_body, 0)

    @pl.when(sp > 0)
    def _():
        rim_copy.wait_recv()

    def local_body(b, carry):
        relay(2 * chunks + b)
        project(4, pg, b * CHUNK)
        at = pl.ds(pl.multiple_of(b * CHUNK, CHUNK), CHUNK)
        for h in range(heads):
            cols = slice(h * HEAD_DIM, (h + 1) * HEAD_DIM)
            q = rotate(pq[at, cols].astype(F32), at).astype(BF16)
            qr[at, cols] = q
            scores = lax.dot_general(
                q, kr[at, cols], (((1,), (1,)), ((), ())), preferred_element_type=F32
            )
            scores = (scores * decay[h]).astype(BF16)
            raw[at, cols] = dot(scores, pv[at, cols]) + qdec[h] * dot(
                q, states[b, h].astype(BF16)
            )
        for s in range(CHUNK // SUB):
            first = b * CHUNK + s * SUB
            here = sp * length + first + lax.broadcasted_iota(jnp.int32, (SUB, GROUP_DIM), 0)
            for g in range(groups):
                cols = slice(g * GROUP_DIM, (g + 1) * GROUP_DIM)
                span = pp[pl.ds(pl.multiple_of(first, SUB), SUB + RIM), cols]
                x = pp[pl.ds(pl.multiple_of(first + RIM, RIM), SUB), cols].astype(F32)
                count = jnp.minimum(here + 1, windows[g]).astype(F32)
                diff = (dot(band[g], span) / count - x).astype(BF16)
                mixed = dot(diff, pool_mix[g]) + pool_bias[g : g + 1]
                pool_out[pl.ds(pl.multiple_of(first, SUB), SUB), cols] = (
                    mixed * pool_gain[:, cols]
                ).astype(BF16)
        return carry

    lax.fori_loop(0, chunks, local_body, 0)

    def rest(h, carry):
        late = (h + HOP * sp >= slots) | (sp == n_sp - 1)

        @pl.when(late & (sp > 0))
        def _():
            relay_head(h)

        return carry

    lax.fori_loop(0, heads, rest, 0)
    for copy in wo_in:
        copy.wait()

    def finish(start, ret):
        at = pl.ds(pl.multiple_of(start, CHUNK), CHUNK)
        for h in range(heads):
            cols = slice(h * HEAD_DIM, (h + 1) * HEAD_DIM)
            ahead = jnp.exp(jnp.full((1, HEAD_DIM), logs[h], F32) * start.astype(F32))
            state = (sin_buf[h].astype(F32) * ahead).astype(BF16)
            r = raw[at, cols] + qdec[h] * dot(qr[at, cols], state)
            r = r - jnp.mean(r, axis=-1, keepdims=True)
            var = jnp.mean(r * r, axis=-1, keepdims=True)
            gate = pg[at, cols].astype(F32)
            gated = gate * (1.0 / (1.0 + jnp.exp(-gate))) * ret_gain[:, cols]
            ret[:, cols] = (
                gated * (r * lax.rsqrt(var + 1e-06))
            ).astype(BF16)

    def part_copy(j):
        at = pl.ds(pl.multiple_of(j * CHUNK, CHUNK), CHUNK)
        return pltpu.make_async_remote_copy(
            src_ref=part_send.at[at],
            dst_ref=part_recv.at[at],
            send_sem=part_ss.at[j],
            recv_sem=part_rs.at[j],
            device_id=peer,
            device_id_type=pl.DeviceIdType.MESH,
        )

    tile = 512

    def multiply(start, ret, dst, j):
        at = pl.ds(pl.multiple_of(start, CHUNK), CHUNK)
        mine = slice(j * CHUNK, (j + 1) * CHUNK)
        left = jnp.concatenate([pool_out[at, :], ret[...]], axis=1)
        for n in range(wide // tile):
            cols = slice(n * tile, (n + 1) * tile)
            dst[mine, cols] = dot(left, wo[:, cols]).astype(BF16)

    starts = [other + j * CHUNK for j in range(per_half)] + [
        own + j * CHUNK for j in range(per_half)
    ]
    rets = (ret_a, ret_b)
    finish(starts[0], ret_a)
    for i, start in enumerate(starts):
        sending = i < per_half
        multiply(start, rets[i % 2], part_send if sending else out_own, i % per_half)
        if i + 1 < len(starts):
            finish(starts[i + 1], rets[(i + 1) % 2])
        if sending:
            part_copy(i).start()

    for j in range(per_half):
        part_copy(j).wait_recv()

    for i in range(PARTS):
        tok_copy(i).wait_send()
    for j in range(per_half):
        part_copy(j).wait_send()

    @pl.when(sp < n_sp - 1)
    def _():
        rim_copy.wait_send()
        for h in range(heads):
            st_copy(h).wait_send()


def per_device(
    tokens,
    norm_gain,
    w_pool,
    w_query,
    w_key,
    w_value,
    w_gate,
    pool_mix,
    pool_bias,
    pool_gain,
    ret_gain,
    w_out_pool,
    w_out_ret,
):
    n_sp, n_tp = lax.axis_size("sp"), lax.axis_size("tp")
    rows, model = tokens.shape
    length = rows * n_tp
    width = w_query.shape[1]
    heads = width // HEAD_DIM
    pool_width = w_pool.shape[1]
    groups = pool_width // GROUP_DIM
    chunks = length // CHUNK
    per_half = rows // CHUNK
    wide = w_out_pool.shape[1]
    hbm = pl.BlockSpec(memory_space=pltpu.HBM)
    vmem = pl.BlockSpec(memory_space=pltpu.VMEM)
    dma = pltpu.SemaphoreType.DMA
    flops = 2 * length * model * (pool_width + 4 * width) + 2 * length * (pool_width + width) * wide
    own, received = pl.pallas_call(
        functools.partial(layer_kernel, n_sp, n_tp),
        out_shape=[pltpu.VMEM((rows, wide), BF16)] * 2,
        in_specs=[hbm, vmem, hbm, hbm, hbm, hbm, hbm, vmem, vmem, vmem, vmem, hbm, hbm],
        out_specs=[vmem, vmem],
        scratch_shapes=[
            pltpu.VMEM((length, model), BF16),
            pltpu.VMEM((5, model, width), BF16),
            pltpu.VMEM((length, width), BF16),
            pltpu.VMEM((length, width), BF16),
            pltpu.VMEM((length + RIM, pool_width), BF16),
            pltpu.VMEM((length, width), BF16),
            pltpu.VMEM((length, width), BF16),
            pltpu.VMEM((pool_width + width, wide), BF16),
            pltpu.VMEM((length, width), BF16),
            pltpu.VMEM((length, width), BF16),
            pltpu.VMEM((length, width), F32),
            pltpu.VMEM((length, pool_width), BF16),
            pltpu.VMEM((CHUNK, width), BF16),
            pltpu.VMEM((CHUNK, width), BF16),
            pltpu.VMEM((length, HEAD_DIM), F32),
            pltpu.VMEM((length, HEAD_DIM), F32),
            pltpu.VMEM((heads, CHUNK, CHUNK), F32),
            pltpu.VMEM((heads, CHUNK, HEAD_DIM), F32),
            pltpu.VMEM((heads, CHUNK, HEAD_DIM), F32),
            pltpu.VMEM((chunks, heads, HEAD_DIM, HEAD_DIM), F32),
            pltpu.VMEM((heads, HEAD_DIM, HEAD_DIM), F32),
            pltpu.VMEM((heads, HEAD_DIM, HEAD_DIM), BF16),
            pltpu.VMEM((heads, HEAD_DIM, HEAD_DIM), BF16),
            pltpu.VMEM((groups, SUB, SUB + RIM), BF16),
            pltpu.VMEM((heads, 8, HEAD_DIM), F32),
            pltpu.VMEM((rows, wide), BF16),
            dma,
            dma((5,)),
            dma((2,)),
            dma((PARTS,)),
            dma((PARTS,)),
            dma((heads,)),
            dma((heads,)),
            dma((2,)),
            dma((per_half,)),
            dma((per_half,)),
        ],
        compiler_params=pltpu.CompilerParams(
            collective_id=0, has_side_effects=True, vmem_limit_bytes=50 * 1024 * 1024
        ),
        cost_estimate=pl.CostEstimate(
            flops=flops, bytes_accessed=20 * 1024 * 1024, transcendentals=0
        ),
    )(
        tokens,
        norm_gain.reshape(1, -1),
        w_pool,
        w_query,
        w_key,
        w_value,
        w_gate,
        pool_mix,
        pool_bias,
        pool_gain.reshape(1, -1),
        ret_gain.reshape(1, -1),
        w_out_pool,
        w_out_ret,
    )
    return (own.astype(F32) + received.astype(F32)).astype(BF16)


def solution(mesh):
    return jax.shard_map(
        per_device,
        mesh=mesh,
        in_specs=(
            P(("fs", "sp", "tp"), None),
            P(),
            P(None, "tp"),
            P(None, "tp"),
            P(None, "tp"),
            P(None, "tp"),
            P(None, "tp"),
            P("tp", None, None),
            P("tp", None),
            P("tp"),
            P("tp"),
            P("tp", None),
            P("tp", None),
        ),
        out_specs=P(("fs", "sp", "tp"), None),
        check_vma=False,
    )
```
